32 devices in a mesh: tp: 8 (over z, y), dp: 4 (over x, core).
Axes of the slice: x: 2, y: 2, z: 4, core: 2. Of those that a mesh axis runs over, the one named last changes fastest.
Arguments:
- tokens: bfloat16 [128, 4096], P('tp', 'dp'), may hold values from -10 to 10
- norm_gain: float32 [2, 4096], P(None, 'dp'), may hold values from 0.1 to 1.9
- input_weight: bfloat16 [2, 4096, 1024], P(None, 'dp', 'tp'), may hold values from -0.09375 to 0.09375
- decay_rate: float32 [2, 64, 64], P(None, 'tp'), may hold values from 0.01 to 1
- frequency: float32 [2, 64, 64], P(None, 'tp'), may hold values from 0.5 to 3
- step_size: float32 [2, 64], P(None, 'tp'), may hold values from 0.1 to 1
- state_in: float32 [2, 64, 16, 128], P(None, 'tp'), may hold values from -1.5 to 1.5
- readout: float32 [2, 64, 16, 128], P(None, 'tp'), may hold values from -0.5 to 0.5
- skip_gain: float32 [2, 1024], P(None, 'tp'), may hold values from -3 to 3
- value_weight: bfloat16 [2, 1024, 4096], P(None, 'tp', 'dp'), may hold values from -0.1875 to 0.1875
- gate_weight: bfloat16 [2, 1024, 4096], P(None, 'tp', 'dp'), may hold values from -0.1875 to 0.1875
- states: float32 [2, 128, 64, 128], P(None, 'dp', 'tp'), may hold values from -3 to 3
Outputs:
- tokens_out: bfloat16 [128, 4096], P('tp', 'dp')
- states_out: float32 [2, 128, 64, 128], P(None, 'dp', 'tp')
The draws below stay inside these ranges and needn't reach their ends.
All inputs are finite; a program needn't handle non-finite values.
Results may differ from the reference program's by a relative error of at most 0.007.
Values may be sent and summed in bfloat16 or wider, within the bound.
No kernel may reach another device: no remote copies, remote signals or barrier semaphores. Data moves between devices by JAX's collectives and lax.ppermute only.
A program may use at most 64 MiB of HBM per device.

```python
import math
import jax
import jax.numpy as jnp
from jax import lax

D = 4096
S = 1024
GS = 16
P_SIZE = 64
LAYERS = 2
G = 64
BATCH = 128


def draw_tokens(key, part):
    first, second, third = jax.random.split(key, 3)
    column_scale = jnp.exp(jax.random.uniform(second, (32,), jnp.float32, -0.7, 0.7))
    column_scale = jnp.repeat(column_scale, D // 32)
    base = jnp.clip(jax.random.normal(first, (BATCH, D), jnp.float32), -4.0, 4.0)
    return (base * column_scale[None, :]).astype(jnp.bfloat16)


def steps_of(stream_key, dims, pieces, smallest, top_value):
    def one(position, blocks):
        steps = jax.random.uniform(jax.random.fold_in(jax.random.fold_in(stream_key, 6), position), (blocks,), jnp.float32, smallest / len(pieces), top_value / len(pieces))
        return jnp.repeat(jnp.exp(steps), dims[position] // blocks).reshape((-1,) + (1,) * (len(dims) - position - 1))

    level = one(*pieces[0])
    for cut in pieces[1:]:
        level = level * one(*cut)
    return level


def bell_draw(stream_key, dims, spread, most, pieces=(), dtype=jnp.bfloat16):
    result = jax.random.normal(stream_key, dims, jnp.float32) * spread
    if len(pieces) > 0:
        result = steps_of(stream_key, dims, pieces, -0.22, 0.18) * result
    return jnp.clip(result, min=-most, max=most).astype(dtype)


def setup_inputs(seed: int = 0) -> dict:
    seeds = jax.random.split(jax.random.key(seed), 13)
    tokens = draw_tokens(jax.random.fold_in(seeds[12], 71), 0)
    norm_gain = jnp.clip(1.0 + 0.18 * jax.random.normal(seeds[1], (LAYERS, D), jnp.float32), 0.1, 1.9)
    input_weight = bell_draw(seeds[2], (LAYERS, D, S), D ** -0.5, 0.09375, ((1, 4), (2, 8)))
    decay_rate = jnp.clip(jnp.exp(math.log(1.0) - 4.6051702 * jax.random.uniform(seeds[3], (LAYERS, G, P_SIZE), jnp.float32) ** steps_of(seeds[3], (LAYERS, G, P_SIZE), ((1, 8),), -0.2, 0.2)), 0.01, 1.0)
    frequency = jnp.clip(0.5 + 2.5 * jax.random.uniform(seeds[4], (LAYERS, G, P_SIZE), jnp.float32) ** steps_of(seeds[4], (LAYERS, G, P_SIZE), ((1, 8),), -0.2, 0.2), 0.5, 3.0)
    step_size = jnp.clip(jnp.exp(math.log(1.0) - 2.3025851 * jax.random.uniform(seeds[5], (LAYERS, G), jnp.float32) ** steps_of(seeds[5], (LAYERS, G), ((1, 8),), -0.2, 0.2)), 0.1, 1.0)
    state_in = bell_draw(seeds[6], (LAYERS, G, GS, 2 * P_SIZE), GS ** -0.5, 1.5, ((1, 8),), jnp.float32)
    readout = bell_draw(seeds[7], (LAYERS, G, GS, 2 * P_SIZE), (2 * P_SIZE) ** -0.5, 0.5, ((1, 8),), jnp.float32)
    skip_gain = bell_draw(seeds[8], (LAYERS, S), 0.5, 3.0, ((1, 8),), jnp.float32)
    value_weight = bell_draw(seeds[9], (LAYERS, S, D), S ** -0.5, 0.1875, ((1, 8), (2, 4)))
    gate_weight = bell_draw(seeds[10], (LAYERS, S, D), S ** -0.5, 0.1875, ((1, 8), (2, 4)))
    states = bell_draw(seeds[11], (LAYERS, BATCH, G, 2 * P_SIZE), 0.5, 3.0, ((1, 4), (2, 8)), jnp.float32)
    return dict(tokens=tokens, norm_gain=norm_gain, input_weight=input_weight, decay_rate=decay_rate, frequency=frequency, step_size=step_size, state_in=state_in, readout=readout, skip_gain=skip_gain, value_weight=value_weight, gate_weight=gate_weight, states=states)


epsilon = 1e-06

def transition(rate, frequency, step):
    magnitude = jnp.exp(-rate * step[:, None])
    angle = frequency * step[:, None]
    keep_real = magnitude * jnp.cos(angle)
    keep_imag = magnitude * jnp.sin(angle)
    minus_one = keep_real - 1.0
    denominator = rate * rate + frequency * frequency
    lift_real = (-minus_one * rate + keep_imag * frequency) / denominator
    lift_imag = (-keep_imag * rate - minus_one * frequency) / denominator
    return (keep_real, keep_imag, lift_real, lift_imag)

def update(drive, state, rate, frequency, step, state_in, readout, skip):
    groups = rate.shape[0]
    half = state.shape[-1] // 2
    grouped = drive.reshape(drive.shape[0], groups, -1)
    pushed = jnp.einsum('sgc,gcq->sgq', grouped, state_in, precision=lax.Precision.HIGHEST)
    keep_real, keep_imag, lift_real, lift_imag = transition(rate, frequency, step)
    push_real, push_imag = (pushed[..., :half], pushed[..., half:])
    old_real, old_imag = (state[..., :half], state[..., half:])
    new_real = keep_real * old_real - keep_imag * old_imag + lift_real * push_real - lift_imag * push_imag
    new_imag = keep_real * old_imag + keep_imag * old_real + lift_real * push_imag + lift_imag * push_real
    new_state = jnp.concatenate([new_real, new_imag], axis=-1)
    summed = jnp.einsum('sgq,gcq->sgc', new_state, readout, precision=lax.Precision.HIGHEST)
    value = summed.reshape(drive.shape) + skip[None, :] * drive
    return (new_state, jax.nn.gelu(value).astype(jnp.bfloat16))

def reference(tokens, norm_gain, input_weight, decay_rate, frequency, step_size, state_in, readout, skip_gain, value_weight, gate_weight, states):
    current = tokens
    updated = []
    for depth_index in range(LAYERS):
        widened = current.astype(jnp.float32)
        mean_square = lax.optimization_barrier(jnp.mean(widened * widened, axis=1))
        gained = (widened * norm_gain[depth_index][None, :]).astype(jnp.bfloat16)
        drive = jnp.dot(gained, input_weight[depth_index], preferred_element_type=jnp.float32)
        drive = drive * lax.rsqrt(mean_square + epsilon)[:, None]
        new_state, readout_value = update(drive, states[depth_index], decay_rate[depth_index], frequency[depth_index], step_size[depth_index], state_in[depth_index], readout[depth_index], skip_gain[depth_index])
        updated.append(new_state)
        value = jnp.dot(readout_value, value_weight[depth_index], preferred_element_type=jnp.float32)
        gate = jnp.dot(readout_value, gate_weight[depth_index], preferred_element_type=jnp.float32)
        current = (widened + value * jax.nn.sigmoid(gate)).astype(jnp.bfloat16)
    return (current, jnp.stack(updated))
```

```python
import jax
import jax.numpy as jnp
from jax import lax
from jax.sharding import PartitionSpec as P

LAYERS = 2


epsilon = 1e-06


def transition(rate, frequency, step):
    magnitude = jnp.exp(-rate * step[:, None])
    angle = frequency * step[:, None]
    keep_real = magnitude * jnp.cos(angle)
    keep_imag = magnitude * jnp.sin(angle)
    minus_one = keep_real - 1.0
    denominator = rate * rate + frequency * frequency
    lift_real = (-minus_one * rate + keep_imag * frequency) / denominator
    lift_imag = (-keep_imag * rate - minus_one * frequency) / denominator
    return (keep_real, keep_imag, lift_real, lift_imag)


def update(drive, state, rate, frequency, step, state_in, readout, skip):
    groups = rate.shape[0]
    half = state.shape[-1] // 2
    grouped = drive.reshape(drive.shape[0], groups, -1)
    pushed = jnp.einsum("sgc,gcq->sgq", grouped, state_in, precision=lax.Precision.HIGHEST)
    keep_real, keep_imag, lift_real, lift_imag = transition(rate, frequency, step)
    push_real, push_imag = (pushed[..., :half], pushed[..., half:])
    old_real, old_imag = (state[..., :half], state[..., half:])
    new_real = (
        keep_real * old_real - keep_imag * old_imag + lift_real * push_real - lift_imag * push_imag
    )
    new_imag = (
        keep_real * old_imag + keep_imag * old_real + lift_real * push_imag + lift_imag * push_real
    )
    new_state = jnp.concatenate([new_real, new_imag], axis=-1)
    summed = jnp.einsum("sgq,gcq->sgc", new_state, readout, precision=lax.Precision.HIGHEST)
    value = summed.reshape(drive.shape) + skip[None, :] * drive
    return (new_state, jax.nn.gelu(value).astype(jnp.bfloat16))


def partner_of(index, shift, count):
    if count & (count - 1) == 0:
        return index ^ shift
    return (index + shift) % count


def source_of(index, shift, count):
    if count & (count - 1) == 0:
        return index ^ shift
    return (index - shift) % count


def send(block, axis, shift, count):
    return lax.ppermute(block, axis, [(s, partner_of(s, shift, count)) for s in range(count)])


def scatter_sum(blocks, axis):
    count = blocks.shape[0]
    own = lax.axis_index(axis)
    total = lax.dynamic_index_in_dim(blocks, own, 0, False)
    for shift in range(1, count):
        block = lax.dynamic_index_in_dim(blocks, partner_of(own, shift, count), 0, False)
        total = total + send(block, axis, shift, count)
    return total


def gather(block, axis):
    count = lax.axis_size(axis)
    own = lax.axis_index(axis)
    whole = jnp.zeros((count,) + block.shape, block.dtype)
    whole = lax.dynamic_update_index_in_dim(whole, block, own, 0)
    for shift in range(1, count):
        got = send(block, axis, shift, count)
        whole = lax.dynamic_update_index_in_dim(whole, got, source_of(own, shift, count), 0)
    return whole


def body(
    tokens,
    norm_gain,
    input_weight,
    decay_rate,
    frequency,
    step_size,
    state_in,
    readout,
    skip_gain,
    value_weight,
    gate_weight,
    states,
):
    current = tokens
    own_rows = states.shape[1]
    tp = lax.axis_size("tp")
    dp = lax.axis_size("dp")
    features = tokens.shape[1] * dp
    rows = tokens.shape[0]
    width_dev = tokens.shape[1]
    updated = []
    for depth_index in range(LAYERS):
        copies = jnp.broadcast_to(current[None], (tp,) + current.shape)
        whole = lax.all_to_all(copies, "tp", 0, 0, tiled=True).reshape(tp * rows, width_dev)
        widened = whole.astype(jnp.float32)
        squares = jnp.sum(widened * widened, axis=1)
        gained = (widened * norm_gain[depth_index][None, :]).astype(jnp.bfloat16)
        summed = jnp.dot(gained, input_weight[depth_index], preferred_element_type=jnp.float32)
        channels = summed.shape[1]
        extra = jnp.broadcast_to(squares.reshape(dp, 1, own_rows), (dp, 8, own_rows))
        extra = jnp.pad(extra, ((0, 0), (0, 0), (0, channels - own_rows)))
        blocks = jnp.concatenate([summed.reshape(dp, own_rows, channels), extra], axis=1)
        totals = scatter_sum(blocks, "dp")
        own_squares = totals[own_rows, :own_rows]
        drive = totals[:own_rows] * lax.rsqrt(own_squares / features + epsilon)[:, None]
        new_state, readout_value = update(
            drive,
            states[depth_index],
            decay_rate[depth_index],
            frequency[depth_index],
            step_size[depth_index],
            state_in[depth_index],
            readout[depth_index],
            skip_gain[depth_index],
        )
        updated.append(new_state)
        ready = gather(readout_value, "dp").reshape(dp * own_rows, channels)
        value = jnp.dot(ready, value_weight[depth_index], preferred_element_type=jnp.float32)
        gate = jnp.dot(ready, gate_weight[depth_index], preferred_element_type=jnp.float32)
        both = jnp.concatenate([value.astype(jnp.bfloat16), gate.astype(jnp.bfloat16)], axis=1)
        parts = lax.all_to_all(both.reshape(tp, rows, 2 * width_dev), "tp", 0, 0, tiled=True)
        both = jnp.sum(parts.astype(jnp.float32), axis=0)
        value, gate = (both[:, :width_dev], both[:, width_dev:])
        current = (current.astype(jnp.float32) + value * jax.nn.sigmoid(gate)).astype(jnp.bfloat16)
    return (current, jnp.stack(updated))


def solution(mesh):
    in_specs = (
        P("tp", "dp"),
        P(None, "dp"),
        P(None, "dp", "tp"),
        P(None, "tp", None),
        P(None, "tp", None),
        P(None, "tp"),
        P(None, "tp", None, None),
        P(None, "tp", None, None),
        P(None, "tp"),
        P(None, "tp", "dp"),
        P(None, "tp", "dp"),
        P(None, "dp", "tp", None),
    )
    out_specs = (P("tp", "dp"), P(None, "dp", "tp", None))
    return jax.shard_map(body, mesh=mesh, in_specs=in_specs, out_specs=out_specs, check_vma=False)
```

```python
import jax
import jax.numpy as jnp
from jax import lax
from jax.sharding import PartitionSpec as P

LAYERS = 2


epsilon = 1e-06


def transition(rate, frequency, step):
    magnitude = jnp.exp(-rate * step[:, None])
    angle = frequency * step[:, None]
    keep_real = magnitude * jnp.cos(angle)
    keep_imag = magnitude * jnp.sin(angle)
    minus_one = keep_real - 1.0
    denominator = rate * rate + frequency * frequency
    lift_real = (-minus_one * rate + keep_imag * frequency) / denominator
    lift_imag = (-keep_imag * rate - minus_one * frequency) / denominator
    return (keep_real, keep_imag, lift_real, lift_imag)


def swap(block, axis, mask):
    count = lax.axis_size(axis)
    return lax.ppermute(block, axis, [(s, s ^ mask) for s in range(count)])


def masks(count):
    if count & (count - 1):
        raise ValueError("axis size")
    return [1 << bit for bit in range(count.bit_length() - 1)]


def gather(block, axis, stride, count):
    place = (lax.axis_index(axis) // stride) % count
    whole = jnp.zeros((count,) + block.shape, block.dtype)
    whole = lax.dynamic_update_index_in_dim(whole, block, place, 0)
    for mask in range(count - 1, 0, -1):
        got = swap(block, axis, mask * stride)
        whole = lax.dynamic_update_index_in_dim(whole, got, place ^ mask, 0)
    return whole


def scatter_sum(blocks, axis, stride, count, dimension):
    place = (lax.axis_index(axis) // stride) % count
    total = lax.dynamic_index_in_dim(blocks, place, dimension, False).astype(jnp.float32)
    for mask in range(count - 1, 0, -1):
        block = lax.dynamic_index_in_dim(blocks, place ^ mask, dimension, False)
        total = total + swap(block, axis, mask * stride).astype(jnp.float32)
    return total


def fold(values, width):
    pieces = []
    for first in range(0, values.shape[1], width):
        piece = values[:, first : first + width]
        pieces.append(jnp.pad(piece, ((0, 0), (0, width - piece.shape[1]))))
    return pieces


def unfold(values, shape):
    pieces = [values[first : first + shape[0]] for first in range(0, values.shape[0], shape[0])]
    return jnp.concatenate(pieces, axis=1)[:, : shape[1]]


def complex_scale(real, imag, values):
    half = values.shape[-1] // 2
    first, second = (values[..., :half], values[..., half:])
    return jnp.concatenate(
        [real * first - imag * second, real * second + imag * first], axis=-1
    )


def body(
    tokens,
    norm_gain,
    input_weight,
    decay_rate,
    frequency,
    step_size,
    state_in,
    readout,
    skip_gain,
    value_weight,
    gate_weight,
    states,
):
    current = tokens
    own_rows, groups = states.shape[1:3]
    tp = lax.axis_size("tp")
    dp = lax.axis_size("dp")
    inner = 1 << (len(masks(tp)) // 2)
    outer = tp // inner
    rows, width_dev = tokens.shape
    features = width_dev * dp
    channels = groups * state_in.shape[2]
    start = lax.axis_index("dp") * own_rows
    group_of = lax.broadcasted_iota(jnp.int32, (channels, channels), 0) // state_in.shape[2]
    other_group = lax.broadcasted_iota(jnp.int32, (channels, channels), 1) // state_in.shape[2]
    row = lax.broadcasted_iota(jnp.int32, (channels, channels), 0)
    column = lax.broadcasted_iota(jnp.int32, (channels, channels), 1)
    kept, lifted, mixers, held = ([], [], [], [])
    pair = gather(current, "tp", 1, inner)
    pair, decay_rate, frequency, step_size = lax.optimization_barrier(
        (pair, decay_rate, frequency, step_size)
    )
    for depth_index in range(LAYERS):
        keep_real, keep_imag, lift_real, lift_imag = transition(
            decay_rate[depth_index], frequency[depth_index], step_size[depth_index]
        )
        keep_state = complex_scale(keep_real, keep_imag, states[depth_index])
        lift_in = complex_scale(lift_real[:, None], lift_imag[:, None], state_in[depth_index])
        cross = lax.dot_general(
            lift_in.reshape(channels, -1),
            readout[depth_index].reshape(channels, -1),
            (((1,), (1,)), ((), ())),
            precision=lax.Precision.HIGHEST,
            preferred_element_type=jnp.float32,
        )
        mixer = jnp.where(group_of == other_group, cross, 0.0)
        mixers.append(mixer + jnp.where(row == column, skip_gain[depth_index][None, :], 0.0))
        base = jnp.einsum(
            "sgq,gcq->sgc", keep_state, readout[depth_index], precision=lax.Precision.HIGHEST
        )
        held.append(base.reshape(own_rows, channels))
        kept.append(keep_state)
        lifted.append(lift_in)
    updated = []
    for depth_index in range(LAYERS):
        if depth_index:
            pair = gather(current, "tp", 1, inner)
        whole = gather(pair, "tp", inner, outer).reshape(tp * rows, width_dev)
        widened = whole.astype(jnp.float32)
        gained = (widened * norm_gain[depth_index][None, :]).astype(jnp.bfloat16)
        squares = lax.dot_general(
            jnp.ones((8, width_dev), jnp.float32),
            widened * widened,
            (((1,), (1,)), ((), ())),
            precision=lax.Precision.HIGHEST,
            preferred_element_type=jnp.float32,
        )
        total = jnp.dot(gained, input_weight[depth_index], preferred_element_type=jnp.float32)
        base = held[depth_index]
        for mask in masks(dp):
            upper = squares.astype(jnp.bfloat16)
            lower = (squares - upper.astype(jnp.float32)).astype(jnp.bfloat16)
            pieces = [total.astype(jnp.bfloat16), base.astype(jnp.bfloat16)]
            packed = jnp.concatenate(pieces + fold(upper, channels) + fold(lower, channels), axis=0)
            got = swap(packed, "dp", mask).astype(jnp.float32)
            total = total + got[: tp * rows]
            edge = tp * rows + base.shape[0]
            middle = (got.shape[0] + edge) // 2
            squares = squares + unfold(got[edge:middle] + got[middle:], squares.shape)
            got = got[tp * rows : edge]
            late = (lax.axis_index("dp") & mask) != 0
            base = jnp.concatenate([jnp.where(late, got, base), jnp.where(late, base, got)], axis=0)
        drive = total * lax.rsqrt(squares[0] / features + epsilon)[:, None]
        mixed = base + jnp.dot(drive, mixers[depth_index], precision=lax.Precision.HIGHEST)
        ready = jax.nn.gelu(mixed).astype(jnp.bfloat16)
        own_drive = lax.dynamic_slice_in_dim(drive, start, own_rows).reshape(own_rows, groups, -1)
        lift_push = jnp.einsum(
            "sgc,gcq->sgq", own_drive, lifted[depth_index], precision=lax.Precision.HIGHEST
        )
        updated.append(kept[depth_index] + lift_push)
        value = jnp.dot(ready, value_weight[depth_index], preferred_element_type=jnp.float32)
        gate = jnp.dot(ready, gate_weight[depth_index], preferred_element_type=jnp.float32)
        both = jnp.concatenate([value.astype(jnp.bfloat16), gate.astype(jnp.bfloat16)], axis=1)
        blocks = both.reshape(outer, inner, rows, 2 * width_dev)
        halves = scatter_sum(blocks, "tp", 1, inner, 1).astype(jnp.bfloat16)
        both = scatter_sum(halves, "tp", inner, outer, 0)
        value, gate = (both[:, :width_dev], both[:, width_dev:])
        current = (current.astype(jnp.float32) + value * jax.nn.sigmoid(gate)).astype(jnp.bfloat16)
    return (current, jnp.stack(updated))


def solution(mesh):
    in_specs = (
        P("tp", "dp"),
        P(None, "dp"),
        P(None, "dp", "tp"),
        P(None, "tp", None),
        P(None, "tp", None),
        P(None, "tp"),
        P(None, "tp", None, None),
        P(None, "tp", None, None),
        P(None, "tp"),
        P(None, "tp", "dp"),
        P(None, "tp", "dp"),
        P(None, "dp", "tp", None),
    )
    out_specs = (P("tp", "dp"), P(None, "dp", "tp", None))
    return jax.shard_map(body, mesh=mesh, in_specs=in_specs, out_specs=out_specs, check_vma=False)
```

```python
import jax
import jax.numpy as jnp
from jax import lax
from jax.sharding import PartitionSpec as P

LAYERS = 2


epsilon = 1e-06


def transition(rate, frequency, step):
    magnitude = jnp.exp(-rate * step[:, None])
    angle = frequency * step[:, None]
    keep_real = magnitude * jnp.cos(angle)
    keep_imag = magnitude * jnp.sin(angle)
    minus_one = keep_real - 1.0
    denominator = rate * rate + frequency * frequency
    lift_real = (-minus_one * rate + keep_imag * frequency) / denominator
    lift_imag = (-keep_imag * rate - minus_one * frequency) / denominator
    return (keep_real, keep_imag, lift_real, lift_imag)


def swap(block, axis, mask):
    count = lax.axis_size(axis)
    return lax.ppermute(block, axis, [(s, s ^ mask) for s in range(count)])


def masks(count):
    if count & (count - 1):
        raise ValueError("axis size")
    return [1 << bit for bit in range(count.bit_length() - 1)]


def gather(block, axis, stride, count):
    place = (lax.axis_index(axis) // stride) % count
    whole = jnp.zeros((count,) + block.shape, block.dtype)
    whole = lax.dynamic_update_index_in_dim(whole, block, place, 0)
    for mask in range(count - 1, 0, -1):
        got = swap(block, axis, mask * stride)
        whole = lax.dynamic_update_index_in_dim(whole, got, place ^ mask, 0)
    return whole


def scatter_sum(blocks, axis, stride, count, dimension):
    place = (lax.axis_index(axis) // stride) % count
    total = lax.dynamic_index_in_dim(blocks, place, dimension, False).astype(jnp.float32)
    for mask in range(count - 1, 0, -1):
        block = lax.dynamic_index_in_dim(blocks, place ^ mask, dimension, False)
        total = total + swap(block, axis, mask * stride).astype(jnp.float32)
    return total


def fold(values, width):
    pieces = []
    for first in range(0, values.shape[1], width):
        piece = values[:, first : first + width]
        pieces.append(jnp.pad(piece, ((0, 0), (0, width - piece.shape[1]))))
    return pieces


def unfold(values, shape):
    pieces = [values[first : first + shape[0]] for first in range(0, values.shape[0], shape[0])]
    return jnp.concatenate(pieces, axis=1)[:, : shape[1]]


def complex_scale(real, imag, values):
    half = values.shape[-1] // 2
    first, second = (values[..., :half], values[..., half:])
    return jnp.concatenate(
        [real * first - imag * second, real * second + imag * first], axis=-1
    )


def body(
    tokens,
    norm_gain,
    input_weight,
    decay_rate,
    frequency,
    step_size,
    state_in,
    readout,
    skip_gain,
    value_weight,
    gate_weight,
    states,
):
    current = tokens
    own_rows, groups = states.shape[1:3]
    tp = lax.axis_size("tp")
    dp = lax.axis_size("dp")
    inner = 1 << (len(masks(tp)) // 2)
    outer = tp // inner
    rows, width_dev = tokens.shape
    features = width_dev * dp
    channels = groups * state_in.shape[2]
    start = lax.axis_index("dp") * own_rows
    group_of = lax.broadcasted_iota(jnp.int32, (channels, channels), 0) // state_in.shape[2]
    other_group = lax.broadcasted_iota(jnp.int32, (channels, channels), 1) // state_in.shape[2]
    row = lax.broadcasted_iota(jnp.int32, (channels, channels), 0)
    column = lax.broadcasted_iota(jnp.int32, (channels, channels), 1)
    kept, lifted, mixers, held = ([], [], [], [])
    pair = gather(current, "tp", 1, inner)
    pair, decay_rate, frequency, step_size, states, state_in, readout, skip_gain = (
        lax.optimization_barrier(
            (pair, decay_rate, frequency, step_size, states, state_in, readout, skip_gain)
        )
    )
    for depth_index in range(LAYERS):
        keep_real, keep_imag, lift_real, lift_imag = transition(
            decay_rate[depth_index], frequency[depth_index], step_size[depth_index]
        )
        keep_state = complex_scale(keep_real, keep_imag, states[depth_index])
        lift_in = complex_scale(lift_real[:, None], lift_imag[:, None], state_in[depth_index])
        cross = lax.dot_general(
            lift_in.reshape(channels, -1),
            readout[depth_index].reshape(channels, -1),
            (((1,), (1,)), ((), ())),
            precision=lax.Precision.HIGHEST,
            preferred_element_type=jnp.float32,
        )
        mixer = jnp.where(group_of == other_group, cross, 0.0)
        mixers.append(mixer + jnp.where(row == column, skip_gain[depth_index][None, :], 0.0))
        base = jnp.einsum(
            "sgq,gcq->sgc", keep_state, readout[depth_index], precision=lax.Precision.HIGHEST
        )
        held.append(base.reshape(own_rows, channels))
        kept.append(keep_state)
        lifted.append(lift_in)
    updated = []
    for depth_index in range(LAYERS):
        if depth_index:
            pair = gather(current, "tp", 1, inner)
        whole = gather(pair, "tp", inner, outer).reshape(tp * rows, width_dev)
        widened = whole.astype(jnp.float32)
        gained = (widened * norm_gain[depth_index][None, :]).astype(jnp.bfloat16)
        squares = lax.dot_general(
            jnp.ones((8, width_dev), jnp.float32),
            widened * widened,
            (((1,), (1,)), ((), ())),
            precision=lax.Precision.HIGH,
            preferred_element_type=jnp.float32,
        )
        total = jnp.dot(gained, input_weight[depth_index], preferred_element_type=jnp.float32)
        base = held[depth_index]
        for mask in masks(dp):
            upper = squares.astype(jnp.bfloat16)
            lower = (squares - upper.astype(jnp.float32)).astype(jnp.bfloat16)
            pieces = [total.astype(jnp.bfloat16), base.astype(jnp.bfloat16)]
            packed = jnp.concatenate(pieces + fold(upper, channels) + fold(lower, channels), axis=0)
            got = swap(packed, "dp", mask).astype(jnp.float32)
            total = total + got[: tp * rows]
            edge = tp * rows + base.shape[0]
            middle = (got.shape[0] + edge) // 2
            squares = squares + unfold(got[edge:middle] + got[middle:], squares.shape)
            got = got[tp * rows : edge]
            late = (lax.axis_index("dp") & mask) != 0
            base = jnp.concatenate([jnp.where(late, got, base), jnp.where(late, base, got)], axis=0)
        drive = total * lax.rsqrt(squares[0] / features + epsilon)[:, None]
        mixed = base + jnp.dot(drive, mixers[depth_index], precision=lax.Precision.HIGHEST)
        ready = jax.nn.gelu(mixed).astype(jnp.bfloat16)
        own_drive = lax.dynamic_slice_in_dim(drive, start, own_rows).reshape(own_rows, groups, -1)
        lift_push = jnp.einsum(
            "sgc,gcq->sgq", own_drive, lifted[depth_index], precision=lax.Precision.HIGHEST
        )
        updated.append(kept[depth_index] + lift_push)
        value = jnp.dot(ready, value_weight[depth_index], preferred_element_type=jnp.float32)
        gate = jnp.dot(ready, gate_weight[depth_index], preferred_element_type=jnp.float32)
        both = jnp.concatenate([value.astype(jnp.bfloat16), gate.astype(jnp.bfloat16)], axis=1)
        blocks = both.reshape(outer, inner, rows, 2 * width_dev)
        place = lax.axis_index("tp") // inner
        for mask in range(outer - 1, -1, -1):
            block = lax.dynamic_index_in_dim(blocks, place ^ mask, 0, False)
            half = scatter_sum(block, "tp", 1, inner, 0)
            if mask:
                half = swap(half.astype(jnp.bfloat16), "tp", mask * inner).astype(jnp.float32)
            both = half if mask == outer - 1 else both + half
        value, gate = (both[:, :width_dev], both[:, width_dev:])
        current = (current.astype(jnp.float32) + value * jax.nn.sigmoid(gate)).astype(jnp.bfloat16)
    return (current, jnp.stack(updated))


def solution(mesh):
    in_specs = (
        P("tp", "dp"),
        P(None, "dp"),
        P(None, "dp", "tp"),
        P(None, "tp", None),
        P(None, "tp", None),
        P(None, "tp"),
        P(None, "tp", None, None),
        P(None, "tp", None, None),
        P(None, "tp"),
        P(None, "tp", "dp"),
        P(None, "tp", "dp"),
        P(None, "dp", "tp", None),
    )
    out_specs = (P("tp", "dp"), P(None, "dp", "tp", None))
    return jax.shard_map(body, mesh=mesh, in_specs=in_specs, out_specs=out_specs, check_vma=False)
```
